32 devices in a mesh: sp: 8 (over z, x), tp: 4 (over y, core).
Axes of the slice: x: 2, y: 2, z: 4, core: 2. Of those that a mesh axis runs over, the one named last changes fastest.
Arguments:
- queries: bfloat16 [2048, 1024], P('sp', 'tp'), may hold values from -6 to 6
- keys: bfloat16 [2048, 1024], P('sp', 'tp'), may hold values from -6 to 6
- values: bfloat16 [2048, 2048], P('sp', 'tp'), may hold values from -6 to 6
- gate_code: bfloat16 [2048, 32], P('sp'), may hold values from -5.5 to 5.5
- gate_up: bfloat16 [32, 1024], P(None, 'tp'), may hold values from -1 to 1
- gate_bias: float32 [1024], P('tp'), as said below
- gla_gain: float32 [256], replicated, may hold values from 0.1 to 1.9
- conv_input: bfloat16 [2048, 2048], P('sp', 'tp'), may hold values from -6 to 6
- conv_gate: bfloat16 [2048, 2048], P('sp', 'tp'), may hold values from -6 to 6
- conv_taps: float32 [3, 2048], P(None, 'tp'), may hold values from -3.5 to 3.5
- out_gla: bfloat16 [2048, 2048], P('tp', 'sp'), may hold values from -0.09375 to 0.09375
- out_conv: bfloat16 [2048, 2048], P('tp', 'sp'), may hold values from -0.09375 to 0.09375
Outputs:
- mixed: bfloat16 [2048, 2048], P(('sp', 'tp'))
The draws below stay inside these ranges and needn't reach their ends.
Inputs may be any that keep to these rules, and one draw needn't show every extreme that they name: `gate_bias`: every bias is at least 1.5, so every decay per step lies strictly between 0 and 1.
All inputs are finite; a program needn't handle non-finite values.
Results may differ from the reference program's by a relative error of at most 0.028.
Values may be sent and summed in bfloat16 or wider, within the bound.
A program may use at most 64 MiB of HBM per device.

```python
import math
import jax
import jax.numpy as jnp
from jax import lax

D = 2048
HEAD_TOTAL = 8
KEY_WIDTH = 128
HEAD_V = 256
RANK = 32
CONV = 2048
TAPS = 3
SEGMENT_LENGTH = 64
TOK_DEV = 256
TOKENS = 2048
KEYS = 1024
VALS = 2048
N_SP = 8
N_TP = 4


def draw_gate_code(key, part):
    noise_key, shift_key = jax.random.split(jax.random.fold_in(key, 11))
    block_count = TOKENS // 128
    noise = jnp.clip(jax.random.normal(noise_key, (TOKENS, RANK), jnp.float32), -3.5, 3.5)
    shifts = jax.random.uniform(shift_key, (block_count, 1, RANK), jnp.float32, -1.5, 1.5)
    full = noise.reshape(block_count, 128, RANK) + shifts
    return full.reshape(TOKENS, RANK).astype(jnp.bfloat16)


def draw_gate_bias(key, part):
    pick_key, slow_key, fast_key = jax.random.split(jax.random.fold_in(key, 23), 3)
    base = math.log(TOKENS / 16.0) + 1.5
    slow_head = jax.random.permutation(pick_key, HEAD_TOTAL) < HEAD_TOTAL // 2
    slow_value = base + jax.random.uniform(slow_key, (HEAD_TOTAL, KEY_WIDTH), jnp.float32, -0.5, 0.5)
    fast_value = jax.random.uniform(fast_key, (HEAD_TOTAL, KEY_WIDTH), jnp.float32, 1.5, 2.5)
    chosen = jnp.where(slow_head[:, None], slow_value, fast_value)
    return chosen.reshape(HEAD_TOTAL * KEY_WIDTH).astype(jnp.float32)


def block_levels(own_key, extent, shards, smallest, high):
    level, own = 1.0, jax.random.fold_in(own_key, 6)
    for position, shards_of in shards:
        steps = jnp.exp(jax.random.uniform(jax.random.fold_in(own, position), (shards_of,), jnp.float32, smallest / len(shards), high / len(shards)))
        level = level * jnp.repeat(steps, extent[position] // shards_of).reshape([-1 if axis == position else 1 for axis in range(len(extent))])
    return level


def normal_values(own_key, extent, spread, limit, cuts=(), held_as=jnp.bfloat16):
    values = spread * jax.random.normal(own_key, extent, jnp.float32)
    if cuts:
        values = values * block_levels(own_key, extent, cuts, -0.22, 0.18)
    return jnp.clip(values, -limit, limit).astype(held_as)


def setup_inputs(seed: int = 0) -> dict:
    streams_of = jax.random.split(jax.random.key(seed), 13)
    return {
        "queries": normal_values(streams_of[0], (TOKENS, KEYS), 1.0, 6.0, ((0, 8), (1, 4))),
        "keys": normal_values(streams_of[1], (TOKENS, KEYS), 1.0, 6.0, ((0, 8), (1, 4))),
        "values": normal_values(streams_of[2], (TOKENS, VALS), 1.0, 6.0, ((0, 8), (1, 4))),
        "gate_code": draw_gate_code(jax.random.fold_in(streams_of[12], 71), 0),
        "gate_up": normal_values(streams_of[4], (RANK, KEYS), RANK ** -0.5, 1.0, ((1, 4),)),
        "gate_bias": draw_gate_bias(jax.random.fold_in(streams_of[12], 71), 0),
        "gla_gain": jnp.clip(1.0 + 0.18 * jax.random.normal(streams_of[6], (HEAD_V,), jnp.float32), 0.1, 1.9),
        "conv_input": normal_values(streams_of[7], (TOKENS, CONV), 1.0, 6.0, ((0, 8), (1, 4))),
        "conv_gate": normal_values(streams_of[8], (TOKENS, CONV), 1.0, 6.0, ((0, 8), (1, 4))),
        "conv_taps": normal_values(streams_of[9], (TAPS, CONV), TAPS ** -0.5, 3.5, ((1, 4),), jnp.float32),
        "out_gla": normal_values(streams_of[10], (VALS, D), (VALS + CONV) ** -0.5, 0.09375, ((0, 4), (1, 8))),
        "out_conv": normal_values(streams_of[11], (CONV, D), (VALS + CONV) ** -0.5, 0.09375, ((0, 4), (1, 8))),
    }


softness_divisor = 16.0
epsilon = 1.0

def reference(queries, keys, values, gate_code, gate_up, gate_bias, gla_gain, conv_input, conv_gate, conv_taps, out_gla, out_conv):
    segment_count = TOK_DEV // SEGMENT_LENGTH
    reach_rows = TAPS - 1
    val_group = HEAD_TOTAL * HEAD_V // N_TP
    conv_group = CONV // N_TP

    def per_block(carried, inputs):
        carried_state, last_rows = carried
        query_blk, key_blk, value_blk, code_blk, input_blk, gate_blk = inputs
        gate_score = jnp.dot(code_blk, gate_up, preferred_element_type=jnp.float32) + gate_bias
        decay_logarithm = (jax.nn.log_sigmoid(gate_score) / softness_divisor).reshape(segment_count, SEGMENT_LENGTH, HEAD_TOTAL, KEY_WIDTH)
        inside = jnp.cumsum(decay_logarithm, axis=1)
        seg_total = inside[:, -1]
        key_four = key_blk.reshape(segment_count, SEGMENT_LENGTH, HEAD_TOTAL, KEY_WIDTH).astype(jnp.float32)
        scaled_keys = (key_four * jnp.exp(seg_total[:, None] - inside)).astype(jnp.bfloat16)
        value_four = value_blk.reshape(segment_count, SEGMENT_LENGTH, HEAD_TOTAL, HEAD_V).astype(jnp.float32)
        update = jnp.einsum('nshk,nshv->nhkv', scaled_keys.astype(jnp.float32), value_four)

        def advance(running, segment_pair):
            running = jnp.exp(segment_pair[0])[..., None] * running + segment_pair[1]
            return (running, running)
        carried_state, states = lax.scan(advance, carried_state, (seg_total, update))
        low_states = lax.optimization_barrier(states.astype(jnp.bfloat16)).astype(jnp.float32)
        query_four = query_blk.reshape(segment_count, SEGMENT_LENGTH, HEAD_TOTAL, KEY_WIDTH).astype(jnp.float32)
        readout = jnp.einsum('nshk,nhkv->nshv', query_four, low_states)
        norm_scale = lax.rsqrt(lax.optimization_barrier(jnp.mean(readout * readout, axis=-1, keepdims=True)) + epsilon)
        gla_mix = (readout * norm_scale * gla_gain).astype(jnp.bfloat16).reshape(TOK_DEV, HEAD_TOTAL * HEAD_V)
        extended = jnp.concatenate([last_rows, input_blk], axis=0)
        convolved = jnp.zeros((TOK_DEV, CONV), jnp.float32)
        for offset in range(TAPS):
            convolved = convolved + conv_taps[offset] * extended[offset:offset + TOK_DEV].astype(jnp.float32)
        conv_mix = (gate_blk.astype(jnp.float32) * convolved).astype(jnp.bfloat16)
        summed = jnp.zeros((TOK_DEV, D), jnp.float32)
        for group_index in range(N_TP):
            val_lo = group_index * val_group
            conv_lo = group_index * conv_group
            part_sum = jnp.dot(gla_mix[:, val_lo:val_lo + val_group], out_gla[val_lo:val_lo + val_group], preferred_element_type=jnp.float32)
            part_sum = part_sum + jnp.dot(conv_mix[:, conv_lo:conv_lo + conv_group], out_conv[conv_lo:conv_lo + conv_group], preferred_element_type=jnp.float32)
            summed = summed + lax.optimization_barrier(part_sum.astype(jnp.bfloat16)).astype(jnp.float32)
        return ((carried_state, input_blk[TOK_DEV - reach_rows:]), summed.astype(jnp.bfloat16))

    def blocks(source):
        return source.reshape(N_SP, TOK_DEV, source.shape[-1])
    initial = (jnp.zeros((HEAD_TOTAL, KEY_WIDTH, HEAD_V), jnp.float32), jnp.zeros((reach_rows, CONV), jnp.bfloat16))
    sliced = (blocks(queries), blocks(keys), blocks(values), blocks(gate_code), blocks(conv_input), blocks(conv_gate))
    _, outputs = lax.scan(per_block, initial, sliced)
    return outputs.reshape(TOKENS, D)
```

```python
import functools

import jax
import jax.numpy as jnp
from jax import lax
from jax.experimental import pallas as pl
from jax.experimental.pallas import tpu as pltpu
from jax.sharding import PartitionSpec as P

KEY_WIDTH = 128
HEAD_V = 256
SEGMENT_LENGTH = 64


softness_divisor = 16.0
epsilon = 1.0


def for_sending(x):
    return jax.tree.map(lambda a: a.astype(jnp.bfloat16) if a.dtype == jnp.float32 else a, x)


def from_behind(x, axis, by):
    count = lax.axis_size(axis)
    pairs = [(i, i + by) for i in range(count) if 0 <= i + by < count]
    return lax.ppermute(x, axis, pairs)


def chain(earlier, latter):
    return (earlier[0] * latter[0], latter[0][..., None] * earlier[1] + latter[1])


def per_device(
    queries,
    keys,
    values,
    gate_code,
    gate_up,
    gate_bias,
    gla_gain,
    conv_input,
    conv_gate,
    conv_taps,
    out_gla,
    out_conv,
):
    row_count = queries.shape[0]
    segment_count = row_count // SEGMENT_LENGTH
    head_count = queries.shape[1] // KEY_WIDTH
    gate_score = jnp.dot(gate_code, gate_up, preferred_element_type=jnp.float32) + gate_bias
    decay_logarithm = (jax.nn.log_sigmoid(gate_score) / softness_divisor).reshape(
        segment_count, SEGMENT_LENGTH, head_count, KEY_WIDTH
    )
    inside = jnp.cumsum(decay_logarithm, axis=1)
    seg_total = inside[:, -1]
    key_blocks = keys.reshape(segment_count, SEGMENT_LENGTH, head_count, KEY_WIDTH)
    scaled_keys = (key_blocks * jnp.exp(seg_total[:, None] - inside)).astype(jnp.bfloat16)
    value_blocks = values.reshape(segment_count, SEGMENT_LENGTH, head_count, HEAD_V)
    update = jnp.einsum(
        "nshk,nshv->nhkv", scaled_keys, value_blocks, preferred_element_type=jnp.float32
    )
    through, local_state = lax.associative_scan(chain, (jnp.exp(seg_total), update), axis=0)
    device_decay = through[-1]
    device_state = local_state[-1]
    columns = lax.all_to_all(
        device_state[None].astype(jnp.bfloat16), "sp", split_axis=3, concat_axis=0, tiled=True
    ).astype(jnp.float32)
    decays = lax.all_gather(device_decay[None], "sp", axis=0, tiled=True)
    running = lax.associative_scan(chain, (decays, columns), axis=0)[1]
    before = jnp.concatenate([jnp.zeros_like(running[:1]), running[:-1]], axis=0)
    incoming = lax.all_to_all(
        for_sending(before), "sp", split_axis=0, concat_axis=3, tiled=True
    ).astype(before.dtype)[0]
    states = local_state + through[..., None] * incoming[None]
    query_blocks = queries.reshape(segment_count, SEGMENT_LENGTH, head_count, KEY_WIDTH)
    readout = jnp.einsum(
        "nshk,nhkv->nshv",
        query_blocks,
        states.astype(jnp.bfloat16),
        preferred_element_type=jnp.float32,
    )
    norm_scale = lax.rsqrt(jnp.mean(readout * readout, axis=-1, keepdims=True) + epsilon)
    gla_mix = (
        (readout * norm_scale * gla_gain)
        .astype(jnp.bfloat16)
        .reshape(row_count, head_count * HEAD_V)
    )
    reach_rows = conv_taps.shape[0] - 1
    earlier_rows = from_behind(conv_input[row_count - reach_rows :], "sp", 1)
    extended = jnp.concatenate([earlier_rows, conv_input], axis=0)
    convolved = jnp.zeros(conv_input.shape, jnp.float32)
    for offset in range(reach_rows + 1):
        convolved = convolved + conv_taps[offset] * extended[offset : offset + row_count]
    conv_mix = (conv_gate * convolved).astype(jnp.bfloat16)
    wide_gla, wide_conv = (
        lax.all_gather(out_gla, "sp", axis=1, tiled=True),
        lax.all_gather(out_conv, "sp", axis=1, tiled=True),
    )
    summed = jnp.dot(gla_mix, wide_gla, preferred_element_type=jnp.float32)
    return lax.psum_scatter(
        (summed + jnp.dot(conv_mix, wide_conv, preferred_element_type=jnp.float32)).astype(
            jnp.bfloat16
        ),
        "tp",
        scatter_dimension=0,
        tiled=True,
    )


MESH = pl.DeviceIdType.MESH
LANES = 128
HALO = 16
CHUNKS = 2
SPLIT = 2
BITS = 3


def flipped(index, bit):
    return index + bit - 2 * bit * ((index // bit) % 2)


def fits(mesh):
    return mesh.shape["sp"] == SPLIT**BITS


def kernel(
    n_sp,
    n_tp,
    q_ref,
    k_ref,
    v_ref,
    code_ref,
    up_ref,
    bias_ref,
    gain_ref,
    x_ref,
    cg_ref,
    taps_ref,
    wg_ref,
    wc_ref,
    out_ref,
    halo,
    ext,
    st,
    dec,
    cols,
    bef,
    inc,
    sloc,
    thr,
    mix,
    wbuf,
    cbuf,
    crecv,
    halo_sem,
    a_sem,
    d_sem,
    b_sem,
    w_sem,
    mix_sem,
    c_sem,
):
    s, t = lax.axis_index("sp"), lax.axis_index("tp")
    f32, bf16 = jnp.float32, jnp.bfloat16
    rows, key_cols = q_ref.shape
    seg = SEGMENT_LENGTH
    segs = rows // seg
    heads = key_cols // KEY_WIDTH
    val_rows = HEAD_V // n_sp
    chan, width = wg_ref.shape
    piece = rows // n_tp
    started = []

    def send(src, dst, sems, where):
        copy = pltpu.make_async_remote_copy(
            src_ref=src,
            dst_ref=dst,
            send_sem=sems[0],
            recv_sem=sems[1],
            device_id=where,
            device_id_type=MESH,
        )
        copy.start()
        started.append(copy)
        return copy

    def pair(sem, *index):
        return sem.at[(0, *index)], sem.at[(1, *index)]

    side, low, far = flipped(s, 1), flipped(s, 2), flipped(s, 4)

    barrier = pltpu.get_barrier_semaphore()
    greet = [(lax.rem(s + d, n_sp), t) for d in range(1, n_sp)]
    greet += [(p, lax.rem(t + d, n_tp)) for p in (s, low) for d in range(1, n_tp)]
    for where in greet:
        pl.semaphore_signal(barrier, inc=1, device_id=where, device_id_type=MESH)
    pl.semaphore_wait(barrier, len(greet))

    halo_copy = send(
        x_ref.at[pl.ds(rows - HALO, HALO)], halo, pair(halo_sem), (lax.rem(s + 1, n_sp), t)
    )

    weight = (wc_ref, wg_ref)
    step = chan // CHUNKS
    to_side, to_far, onward = {}, {}, {}

    def send_chunk(half, c):
        part = pl.ds(c * step, step)
        to_far[half, c] = send(
            weight[half].at[part], wbuf.at[half, 1, part], pair(w_sem, 1, half, c), (far, t)
        )
        to_side[half, c] = send(
            weight[half].at[part], wbuf.at[half, 0, part], pair(w_sem, 0, half, c), (side, t)
        )

    def pass_on(half, c):
        part = pl.ds(c * step, step)
        to_far[half, c].wait_recv()
        onward[half, c] = send(
            wbuf.at[half, 1, part], wbuf.at[half, 2, part], pair(w_sem, 2, half, c), (side, t)
        )

    send_chunk(0, 0)

    g = jnp.dot(code_ref[...], up_ref[...], preferred_element_type=f32) + bias_ref[...]
    log_decay = (jnp.minimum(g, 0.0) - jnp.log1p(jnp.exp(-jnp.abs(g)))) / softness_divisor
    row_i = lax.broadcasted_iota(jnp.int32, (seg, seg), 0)
    col_i = lax.broadcasted_iota(jnp.int32, (seg, seg), 1)
    later = (col_i > row_i).astype(f32)
    state = None
    passed = None
    for n in range(segs):
        here = pl.ds(n * seg, seg)
        block = log_decay[n * seg : (n + 1) * seg]
        rest = jnp.dot(
            later, block, preferred_element_type=f32, precision=lax.Precision.HIGHEST
        )
        total = jnp.sum(block, axis=0, keepdims=True)
        scaled = (k_ref[here, :].astype(f32) * jnp.exp(rest)).astype(bf16)
        update = jnp.concatenate(
            [
                lax.dot_general(
                    v_ref[here, pl.ds(h * HEAD_V, HEAD_V)],
                    scaled[:, h * KEY_WIDTH : (h + 1) * KEY_WIDTH],
                    (((0,), (0,)), ((), ())),
                    preferred_element_type=f32,
                )
                for h in range(heads)
            ],
            axis=1,
        )
        if n == 0:
            state, passed = update, total
        else:
            state, passed = jnp.exp(total) * state + update, passed + total
        sloc[n] = state
        thr[n] = jnp.exp(passed)
    st[...] = state.astype(bf16).reshape(st.shape)
    dec[s] = jnp.exp(passed)
    cols[s] = st[s]

    first = []
    for d in range(1, n_sp):
        dst = lax.rem(s + d, n_sp)
        first.append(send(st.at[dst], cols.at[s], pair(a_sem, d - 1), (dst, t)))
        first.append(send(dec.at[s], dec.at[s], pair(d_sem, d - 1), (dst, t)))

    send_chunk(0, 1)

    halo_copy.wait_recv()
    ext[pl.ds(0, HALO), :] = jnp.where(s > 0, halo[...].astype(f32), 0.0)
    ext[pl.ds(HALO, rows), :] = x_ref[...].astype(f32)
    taps = taps_ref.shape[0]
    total = None
    for o in range(taps):
        term = taps_ref[pl.ds(o, 1), :] * ext[pl.ds(HALO - taps + 1 + o, rows), :]
        total = term if total is None else total + term
    mix[0, 0] = (cg_ref[...].astype(f32) * total).astype(bf16)

    for copy in first:
        copy.wait_recv()
    running = jnp.zeros(cols.shape[1:], f32)
    for j in range(n_sp):
        bef[j] = running.astype(bf16)
        if j < n_sp - 1:
            running = dec[j] * running + cols[j].astype(f32)
    inc[s] = bef[s]
    second = []
    for d in range(1, n_sp):
        dst = lax.rem(s + d, n_sp)
        second.append(send(bef.at[dst], inc.at[s], pair(b_sem, d - 1), (dst, t)))

    mix_copies = {0: send(mix.at[0, 0], mix.at[1, 0], pair(mix_sem, 0), (low, t))}
    send_chunk(1, 0)
    pass_on(0, 0)

    for copy in second:
        copy.wait_recv()
    incoming = inc[...].astype(f32).reshape(HEAD_V, key_cols)
    for n in range(segs):
        here = pl.ds(n * seg, seg)
        full = (sloc[n] + thr[n] * incoming).astype(bf16)
        for h in range(heads):
            lanes = slice(h * KEY_WIDTH, (h + 1) * KEY_WIDTH)
            read = lax.dot_general(
                q_ref[here, lanes],
                full[:, lanes],
                (((1,), (1,)), ((), ())),
                preferred_element_type=f32,
            )
            scale = lax.rsqrt(jnp.mean(read * read, axis=-1, keepdims=True) + epsilon)
            mix[0, 1, here, pl.ds(h * HEAD_V, HEAD_V)] = (
                read * scale * gain_ref[...]
            ).astype(bf16)
    mix_copies[1] = send(mix.at[0, 1], mix.at[1, 1], pair(mix_sem, 1), (low, t))
    for c in range(1, CHUNKS):
        send_chunk(1, c)
        pass_on(0, c)

    results = {}

    def product(whose, slot):
        acc = None
        for half in range(2):
            w = weight[half][...] if slot == 0 else wbuf[half, slot - 1]
            term = jnp.dot(mix[whose, half], w, preferred_element_type=f32)
            acc = term if acc is None else acc + term
        cbuf[whose, slot] = acc.astype(bf16)
        for d in range(n_tp - 1, -1, -1):
            if whose == 0 and d == 0:
                continue
            other = lax.rem(t + d, n_tp)
            part = pl.ds(pl.multiple_of(other * piece, piece), piece)
            results[whose, d, slot] = send(
                cbuf.at[whose, slot, part],
                crecv.at[whose, d, slot],
                pair(c_sem, whose, d, slot),
                (low if whose else s, other),
            )

    product(0, 0)
    for half in range(2):
        for c in range(CHUNKS):
            to_side[half, c].wait_recv()
    product(0, 1)
    for c in range(CHUNKS):
        pass_on(1, c)
    for half in range(2):
        mix_copies[half].wait_recv()
    product(1, 0)
    product(1, 1)
    product(1, 2)
    product(0, 2)
    for half in range(2):
        for c in range(CHUNKS):
            onward[half, c].wait_recv()
    product(1, 3)
    product(0, 3)

    mine = pl.ds(pl.multiple_of(t * piece, piece), piece)
    for slot in range(4):
        for whose in range(2):
            total = cbuf[0, slot, mine, :].astype(f32) if whose == 0 else None
            for d in range(n_tp):
                if whose == 0 and d == 0:
                    continue
                results[whose, d, slot].wait_recv()
                term = crecv[whose, d, slot].astype(f32)
                total = term if total is None else total + term
            block = low if whose else s
            if slot % 2:
                block = flipped(block, 1)
            if slot // 2:
                block = flipped(block, 4)
            place = pl.ds(pl.multiple_of(block * width, width), width)
            out_ref[:, place] = total.astype(bf16)
    for copy in started:
        copy.wait_send()


def fused(
    queries,
    keys,
    values,
    gate_code,
    gate_up,
    gate_bias,
    gla_gain,
    conv_input,
    conv_gate,
    conv_taps,
    out_gla,
    out_conv,
):
    n_sp, n_tp = lax.axis_size("sp"), lax.axis_size("tp")
    rows, key_cols = queries.shape
    segs = rows // SEGMENT_LENGTH
    chan, width = out_gla.shape
    bf16, f32 = jnp.bfloat16, jnp.float32
    val_rows = HEAD_V // n_sp
    dma = pltpu.SemaphoreType.DMA
    return pl.pallas_call(
        functools.partial(kernel, n_sp, n_tp),
        out_shape=jax.ShapeDtypeStruct((rows // n_tp, n_sp * width), bf16),
        in_specs=[pl.BlockSpec(memory_space=pltpu.VMEM)] * 12,
        out_specs=pl.BlockSpec(memory_space=pltpu.VMEM),
        scratch_shapes=[
            pltpu.VMEM((HALO, conv_input.shape[1]), bf16),
            pltpu.VMEM((HALO + rows, conv_input.shape[1]), f32),
            pltpu.VMEM((n_sp, val_rows, key_cols), bf16),
            pltpu.VMEM((n_sp, 1, key_cols), f32),
            pltpu.VMEM((n_sp, val_rows, key_cols), bf16),
            pltpu.VMEM((n_sp, val_rows, key_cols), bf16),
            pltpu.VMEM((n_sp, val_rows, key_cols), bf16),
            pltpu.VMEM((segs, HEAD_V, key_cols), f32),
            pltpu.VMEM((segs, 1, key_cols), f32),
            pltpu.VMEM((2, 2, rows, chan), bf16),
            pltpu.VMEM((2, 3, chan, width), bf16),
            pltpu.VMEM((2, 4, rows, width), bf16),
            pltpu.VMEM((2, n_tp, 4, rows // n_tp, width), bf16),
            dma((2,)),
            dma((2, n_sp - 1)),
            dma((2, n_sp - 1)),
            dma((2, n_sp - 1)),
            dma((2, 3, 2, CHUNKS)),
            dma((2, 2)),
            dma((2, 2, n_tp, 4)),
        ],
        compiler_params=pltpu.CompilerParams(
            collective_id=0, has_side_effects=True, vmem_limit_bytes=48 * 1024 * 1024
        ),
    )(
        queries,
        keys,
        values,
        gate_code,
        gate_up,
        gate_bias[None],
        gla_gain[None],
        conv_input,
        conv_gate,
        conv_taps,
        out_gla,
        out_conv,
    )


def solution(mesh):
    in_specs = (
        P("sp", "tp"),
        P("sp", "tp"),
        P("sp", "tp"),
        P("sp", None),
        P(None, "tp"),
        P("tp"),
        P(),
        P("sp", "tp"),
        P("sp", "tp"),
        P(None, "tp"),
        P("tp", "sp"),
        P("tp", "sp"),
    )
    out_specs = P(("sp", "tp"), None)
    return jax.shard_map(
        fused if fits(mesh) else per_device, mesh=mesh, in_specs=in_specs, out_specs=out_specs, check_vma=False
    )
```

```python
import functools

import jax
import jax.numpy as jnp
from jax import lax
from jax.experimental import pallas as pl
from jax.experimental.pallas import tpu as pltpu
from jax.sharding import PartitionSpec as P

KEY_WIDTH = 128
HEAD_V = 256
SEGMENT_LENGTH = 64


softness_divisor = 16.0
epsilon = 1.0


def for_sending(x):
    return jax.tree.map(lambda a: a.astype(jnp.bfloat16) if a.dtype == jnp.float32 else a, x)


def from_behind(x, axis, by):
    count = lax.axis_size(axis)
    pairs = [(i, i + by) for i in range(count) if 0 <= i + by < count]
    return lax.ppermute(x, axis, pairs)


def chain(earlier, latter):
    return (earlier[0] * latter[0], latter[0][..., None] * earlier[1] + latter[1])


def per_device(
    queries,
    keys,
    values,
    gate_code,
    gate_up,
    gate_bias,
    gla_gain,
    conv_input,
    conv_gate,
    conv_taps,
    out_gla,
    out_conv,
):
    row_count = queries.shape[0]
    segment_count = row_count // SEGMENT_LENGTH
    head_count = queries.shape[1] // KEY_WIDTH
    gate_score = jnp.dot(gate_code, gate_up, preferred_element_type=jnp.float32) + gate_bias
    decay_logarithm = (jax.nn.log_sigmoid(gate_score) / softness_divisor).reshape(
        segment_count, SEGMENT_LENGTH, head_count, KEY_WIDTH
    )
    inside = jnp.cumsum(decay_logarithm, axis=1)
    seg_total = inside[:, -1]
    key_blocks = keys.reshape(segment_count, SEGMENT_LENGTH, head_count, KEY_WIDTH)
    scaled_keys = (key_blocks * jnp.exp(seg_total[:, None] - inside)).astype(jnp.bfloat16)
    value_blocks = values.reshape(segment_count, SEGMENT_LENGTH, head_count, HEAD_V)
    update = jnp.einsum(
        "nshk,nshv->nhkv", scaled_keys, value_blocks, preferred_element_type=jnp.float32
    )
    through, local_state = lax.associative_scan(chain, (jnp.exp(seg_total), update), axis=0)
    device_decay = through[-1]
    device_state = local_state[-1]
    columns = lax.all_to_all(
        device_state[None].astype(jnp.bfloat16), "sp", split_axis=3, concat_axis=0, tiled=True
    ).astype(jnp.float32)
    decays = lax.all_gather(device_decay[None], "sp", axis=0, tiled=True)
    running = lax.associative_scan(chain, (decays, columns), axis=0)[1]
    before = jnp.concatenate([jnp.zeros_like(running[:1]), running[:-1]], axis=0)
    incoming = lax.all_to_all(
        for_sending(before), "sp", split_axis=0, concat_axis=3, tiled=True
    ).astype(before.dtype)[0]
    states = local_state + through[..., None] * incoming[None]
    query_blocks = queries.reshape(segment_count, SEGMENT_LENGTH, head_count, KEY_WIDTH)
    readout = jnp.einsum(
        "nshk,nhkv->nshv",
        query_blocks,
        states.astype(jnp.bfloat16),
        preferred_element_type=jnp.float32,
    )
    norm_scale = lax.rsqrt(jnp.mean(readout * readout, axis=-1, keepdims=True) + epsilon)
    gla_mix = (
        (readout * norm_scale * gla_gain)
        .astype(jnp.bfloat16)
        .reshape(row_count, head_count * HEAD_V)
    )
    reach_rows = conv_taps.shape[0] - 1
    earlier_rows = from_behind(conv_input[row_count - reach_rows :], "sp", 1)
    extended = jnp.concatenate([earlier_rows, conv_input], axis=0)
    convolved = jnp.zeros(conv_input.shape, jnp.float32)
    for offset in range(reach_rows + 1):
        convolved = convolved + conv_taps[offset] * extended[offset : offset + row_count]
    conv_mix = (conv_gate * convolved).astype(jnp.bfloat16)
    wide_gla, wide_conv = (
        lax.all_gather(out_gla, "sp", axis=1, tiled=True),
        lax.all_gather(out_conv, "sp", axis=1, tiled=True),
    )
    summed = jnp.dot(gla_mix, wide_gla, preferred_element_type=jnp.float32)
    return lax.psum_scatter(
        (summed + jnp.dot(conv_mix, wide_conv, preferred_element_type=jnp.float32)).astype(
            jnp.bfloat16
        ),
        "tp",
        scatter_dimension=0,
        tiled=True,
    )


MESH = pl.DeviceIdType.MESH
ARGS = 12
LANES = 128
HALO = 16
CHUNKS = 2
SPLIT = 2
BITS = 3


def flipped(index, bit):
    return index + bit - 2 * bit * ((index // bit) % 2)


def fits(mesh):
    return mesh.shape["sp"] == SPLIT**BITS and mesh.shape["tp"] == SPLIT**2


def kernel(
    n_sp,
    n_tp,
    *refs,
):
    sources, out_ref, scratch = refs[:ARGS], refs[ARGS], refs[ARGS + 1 :]
    held, scratch = scratch[:ARGS], scratch[ARGS:]
    body(n_sp, n_tp, sources, held, out_ref, *scratch)


def body(
    n_sp,
    n_tp,
    sources,
    held,
    out_ref,
    in_sem,
    halo,
    ext,
    st,
    dec,
    cols,
    bef,
    inc,
    sloc,
    thr,
    mix,
    wbuf,
    cbuf,
    mrecv,
    csum,
    crecv,
    halo_sem,
    a_sem,
    d_sem,
    b_sem,
    w_sem,
    mix_sem,
    m_sem,
    c_sem,
):
    (
        q_ref,
        k_ref,
        v_ref,
        code_ref,
        up_ref,
        bias_ref,
        gain_ref,
        x_ref,
        cg_ref,
        taps_ref,
        wg_ref,
        wc_ref,
    ) = held
    loads = [pltpu.make_async_copy(a, b, in_sem.at[i]) for i, (a, b) in enumerate(zip(sources, held))]
    loading = list(range(ARGS))

    def need(*which):
        for i in which:
            loads[i].wait()
            loading.remove(i)

    for i in (7, 11, 3, 4, 5, 1, 2, 10, 8, 9, 0, 6):
        loads[i].start()
    s, t = lax.axis_index("sp"), lax.axis_index("tp")
    f32, bf16 = jnp.float32, jnp.bfloat16
    rows, key_cols = q_ref.shape
    seg = SEGMENT_LENGTH
    segs = rows // seg
    heads = key_cols // KEY_WIDTH
    val_rows = HEAD_V // n_sp
    chan, width = wg_ref.shape
    piece = rows // n_tp
    started = []

    def send(src, dst, sems, where):
        copy = pltpu.make_async_remote_copy(
            src_ref=src,
            dst_ref=dst,
            send_sem=sems[0],
            recv_sem=sems[1],
            device_id=where,
            device_id_type=MESH,
        )
        copy.start()
        started.append(copy)
        return copy

    def pair(sem, *index):
        return sem.at[(0, *index)], sem.at[(1, *index)]

    side, low, far = flipped(s, 1), flipped(s, 2), flipped(s, 4)

    barrier = pltpu.get_barrier_semaphore()
    greet = [(lax.rem(s + d, n_sp), t) for d in range(1, n_sp)]
    mate, across = flipped(t, 1), flipped(t, 2)
    greet += [(s, mate), (s, across), (low, across)]
    for where in greet:
        pl.semaphore_signal(barrier, inc=1, device_id=where, device_id_type=MESH)
    pl.semaphore_wait(barrier, len(greet))

    need(7, 11)
    halo_copy = send(
        x_ref.at[pl.ds(rows - HALO, HALO)], halo, pair(halo_sem), (lax.rem(s + 1, n_sp), t)
    )

    weight = (wc_ref, wg_ref)
    step = chan // CHUNKS
    to_side, to_far, onward = {}, {}, {}

    def send_chunk(half, c):
        part = pl.ds(c * step, step)
        to_far[half, c] = send(
            weight[half].at[part], wbuf.at[half, 1, part], pair(w_sem, 1, half, c), (far, t)
        )
        to_side[half, c] = send(
            weight[half].at[part], wbuf.at[half, 0, part], pair(w_sem, 0, half, c), (side, t)
        )

    def pass_on(half, c):
        part = pl.ds(c * step, step)
        to_far[half, c].wait_recv()
        onward[half, c] = send(
            wbuf.at[half, 1, part], wbuf.at[half, 2, part], pair(w_sem, 2, half, c), (side, t)
        )

    send_chunk(0, 0)

    need(3, 4, 5, 1, 2)
    g = (
        lax.dot_general(
            code_ref[...],
            up_ref[...],
            (((0,), (0,)), ((), ())),
            preferred_element_type=f32,
        )
        + bias_ref[...]
    )
    log_decay = (jnp.minimum(g, 0.0) - jnp.log1p(jnp.exp(-jnp.abs(g)))) / softness_divisor
    row_i = lax.broadcasted_iota(jnp.int32, (seg, seg), 0)
    col_i = lax.broadcasted_iota(jnp.int32, (seg, seg), 1)
    later = (col_i > row_i).astype(f32)
    state = None
    passed = None
    for n in range(segs):
        here = pl.ds(n * seg, seg)
        block = log_decay[n * seg : (n + 1) * seg]
        rest = jnp.dot(
            later, block, preferred_element_type=f32, precision=lax.Precision.HIGHEST
        )
        total = jnp.sum(block, axis=0, keepdims=True)
        scaled = (k_ref[here, :].astype(f32) * jnp.exp(rest)).astype(bf16)
        update = jnp.concatenate(
            [
                lax.dot_general(
                    v_ref[here, pl.ds(h * HEAD_V, HEAD_V)],
                    scaled[:, h * KEY_WIDTH : (h + 1) * KEY_WIDTH],
                    (((0,), (0,)), ((), ())),
                    preferred_element_type=f32,
                )
                for h in range(heads)
            ],
            axis=1,
        )
        if n == 0:
            state, passed = update, total
        else:
            state, passed = jnp.exp(total) * state + update, passed + total
        sloc[n] = state
        thr[n] = jnp.exp(passed)
    st[...] = state.astype(bf16).reshape(st.shape)
    dec[s] = jnp.exp(passed)
    cols[s] = st[s]

    first = []
    for d in range(1, n_sp):
        dst = lax.rem(s + d, n_sp)
        first.append(send(st.at[dst], cols.at[s], pair(a_sem, d - 1), (dst, t)))
        first.append(send(dec.at[s], dec.at[s], pair(d_sem, d - 1), (dst, t)))

    send_chunk(0, 1)

    halo_copy.wait_recv()
    need(8, 9)
    ext[pl.ds(0, HALO), :] = jnp.where(s > 0, halo[...].astype(f32), 0.0)
    ext[pl.ds(HALO, rows), :] = x_ref[...].astype(f32)
    taps = taps_ref.shape[0]
    total = None
    for o in range(taps):
        term = taps_ref[pl.ds(o, 1), :] * ext[pl.ds(HALO - taps + 1 + o, rows), :]
        total = term if total is None else total + term
    mix[0, 0] = (cg_ref[...].astype(f32) * total).astype(bf16)

    for copy in first:
        copy.wait_recv()
    running = jnp.zeros(cols.shape[1:], f32)
    for j in range(n_sp):
        bef[j] = running.astype(bf16)
        if j < n_sp - 1:
            running = dec[j] * running + cols[j].astype(f32)
    inc[s] = bef[s]
    second = []
    for d in range(1, n_sp):
        dst = lax.rem(s + d, n_sp)
        second.append(send(bef.at[dst], inc.at[s], pair(b_sem, d - 1), (dst, t)))

    need(10, 0, 6)
    for c in range(CHUNKS):
        send_chunk(1, c)
    mix_copies = {0: send(mix.at[0, 0], mix.at[1, 0], pair(mix_sem, 0), (low, t))}
    pass_on(0, 0)

    for copy in second:
        copy.wait_recv()
    incoming = inc[...].astype(f32).reshape(HEAD_V, key_cols)
    for n in range(segs):
        here = pl.ds(n * seg, seg)
        full = (sloc[n] + thr[n] * incoming).astype(bf16)
        for h in range(heads):
            lanes = slice(h * KEY_WIDTH, (h + 1) * KEY_WIDTH)
            read = lax.dot_general(
                q_ref[here, lanes],
                full[:, lanes],
                (((1,), (1,)), ((), ())),
                preferred_element_type=f32,
            )
            scale = lax.rsqrt(jnp.mean(read * read, axis=-1, keepdims=True) + epsilon)
            mix[0, 1, here, pl.ds(h * HEAD_V, HEAD_V)] = (
                read * scale * gain_ref[...]
            ).astype(bf16)
    mix_copies[1] = send(mix.at[0, 1], mix.at[1, 1], pair(mix_sem, 1), (low, t))
    for c in range(1, CHUNKS):
        pass_on(0, c)

    halves, results = {}, {}

    def rows_of(owner):
        return pl.ds(pl.multiple_of(owner * piece, piece), piece)

    def product(whose, slot):
        acc = None
        for half in range(2):
            w = weight[half][...] if slot == 0 else wbuf[half, slot - 1]
            term = jnp.dot(mix[whose, half], w, preferred_element_type=f32)
            acc = term if acc is None else acc + term
        cbuf[whose, slot] = acc.astype(bf16)
        for dy in (1, 0):
            owner = flipped(across, 1) if dy else mate
            halves[whose, slot, dy] = send(
                cbuf.at[whose, slot, rows_of(owner)],
                mrecv.at[whose, slot, dy],
                pair(m_sem, whose, slot, dy),
                (s, mate),
            )

    def finish(whose, slot):
        for dy in (1, 0):
            owner = across if dy else t
            halves[whose, slot, dy].wait_recv()
            both = cbuf[whose, slot, rows_of(owner), :].astype(f32) + mrecv[
                whose, slot, dy
            ].astype(f32)
            csum[whose, slot, dy] = both.astype(bf16)
            if whose or dy:
                results[whose, slot, dy] = send(
                    csum.at[whose, slot, dy],
                    crecv.at[whose, slot, dy],
                    pair(c_sem, whose, slot, dy),
                    (low if whose else s, owner),
                )

    product(0, 0)
    for half in range(2):
        for c in range(CHUNKS):
            to_side[half, c].wait_recv()
    product(0, 1)
    finish(0, 0)
    finish(0, 1)
    for half in range(2):
        mix_copies[half].wait_recv()
    product(1, 0)
    product(1, 1)
    finish(1, 0)
    finish(1, 1)
    for c in range(CHUNKS):
        pass_on(1, c)
    product(1, 2)
    product(0, 2)
    finish(1, 2)
    finish(0, 2)
    for half in range(2):
        for c in range(CHUNKS):
            onward[half, c].wait_recv()
    product(1, 3)
    product(0, 3)
    finish(1, 3)
    finish(0, 3)

    for slot in range(4):
        for whose in range(2):
            results[whose, slot, 1].wait_recv()
            if whose:
                results[1, slot, 0].wait_recv()
                total = crecv[1, slot, 0].astype(f32)
            else:
                total = csum[0, slot, 0].astype(f32)
            total = total + crecv[whose, slot, 1].astype(f32)
            block = low if whose else s
            if slot % 2:
                block = flipped(block, 1)
            if slot // 2:
                block = flipped(block, 4)
            place = pl.ds(pl.multiple_of(block * width, width), width)
            out_ref[:, place] = total.astype(bf16)
    for copy in started:
        copy.wait_send()


def fused(
    queries,
    keys,
    values,
    gate_code,
    gate_up,
    gate_bias,
    gla_gain,
    conv_input,
    conv_gate,
    conv_taps,
    out_gla,
    out_conv,
):
    n_sp, n_tp = lax.axis_size("sp"), lax.axis_size("tp")
    rows, key_cols = queries.shape
    segs = rows // SEGMENT_LENGTH
    chan, width = out_gla.shape
    bf16, f32 = jnp.bfloat16, jnp.float32
    val_rows = HEAD_V // n_sp
    dma = pltpu.SemaphoreType.DMA
    operands = (
        queries,
        keys,
        values,
        gate_code.T,
        gate_up,
        gate_bias[None],
        gla_gain[None],
        conv_input,
        conv_gate,
        conv_taps,
        out_gla,
        out_conv,
    )
    return pl.pallas_call(
        functools.partial(kernel, n_sp, n_tp),
        out_shape=jax.ShapeDtypeStruct((rows // n_tp, n_sp * width), bf16),
        in_specs=[pl.BlockSpec(memory_space=pltpu.HBM)] * ARGS,
        out_specs=pl.BlockSpec(memory_space=pltpu.VMEM),
        scratch_shapes=[
            *(pltpu.VMEM(a.shape, a.dtype) for a in operands),
            dma((ARGS,)),
            pltpu.VMEM((HALO, conv_input.shape[1]), bf16),
            pltpu.VMEM((HALO + rows, conv_input.shape[1]), f32),
            pltpu.VMEM((n_sp, val_rows, key_cols), bf16),
            pltpu.VMEM((n_sp, 1, key_cols), f32),
            pltpu.VMEM((n_sp, val_rows, key_cols), bf16),
            pltpu.VMEM((n_sp, val_rows, key_cols), bf16),
            pltpu.VMEM((n_sp, val_rows, key_cols), bf16),
            pltpu.VMEM((segs, HEAD_V, key_cols), f32),
            pltpu.VMEM((segs, 1, key_cols), f32),
            pltpu.VMEM((2, 2, rows, chan), bf16),
            pltpu.VMEM((2, 3, chan, width), bf16),
            pltpu.VMEM((2, 4, rows, width), bf16),
            pltpu.VMEM((2, 4, 2, rows // n_tp, width), bf16),
            pltpu.VMEM((2, 4, 2, rows // n_tp, width), bf16),
            pltpu.VMEM((2, 4, 2, rows // n_tp, width), bf16),
            dma((2,)),
            dma((2, n_sp - 1)),
            dma((2, n_sp - 1)),
            dma((2, n_sp - 1)),
            dma((2, 3, 2, CHUNKS)),
            dma((2, 2)),
            dma((2, 2, 4, 2)),
            dma((2, 2, 4, 2)),
        ],
        compiler_params=pltpu.CompilerParams(
            collective_id=0, has_side_effects=True, vmem_limit_bytes=67043328
        ),
    )(*operands)


def solution(mesh):
    in_specs = (
        P("sp", "tp"),
        P("sp", "tp"),
        P("sp", "tp"),
        P("sp", None),
        P(None, "tp"),
        P("tp"),
        P(),
        P("sp", "tp"),
        P("sp", "tp"),
        P(None, "tp"),
        P("tp", "sp"),
        P("tp", "sp"),
    )
    out_specs = P(("sp", "tp"), None)
    return jax.shard_map(
        fused if fits(mesh) else per_device, mesh=mesh, in_specs=in_specs, out_specs=out_specs, check_vma=False
    )
```

```python
import functools

import jax
import jax.numpy as jnp
from jax import lax
from jax.experimental import pallas as pl
from jax.experimental.pallas import tpu as pltpu
from jax.sharding import PartitionSpec as P

KEY_WIDTH = 128
HEAD_V = 256
SEGMENT_LENGTH = 64


softness_divisor = 16.0
epsilon = 1.0


def for_sending(x):
    return jax.tree.map(lambda a: a.astype(jnp.bfloat16) if a.dtype == jnp.float32 else a, x)


def from_behind(x, axis, by):
    count = lax.axis_size(axis)
    pairs = [(i, i + by) for i in range(count) if 0 <= i + by < count]
    return lax.ppermute(x, axis, pairs)


def chain(earlier, latter):
    return (earlier[0] * latter[0], latter[0][..., None] * earlier[1] + latter[1])


def per_device(
    queries,
    keys,
    values,
    gate_code,
    gate_up,
    gate_bias,
    gla_gain,
    conv_input,
    conv_gate,
    conv_taps,
    out_gla,
    out_conv,
):
    row_count = queries.shape[0]
    segment_count = row_count // SEGMENT_LENGTH
    head_count = queries.shape[1] // KEY_WIDTH
    gate_score = jnp.dot(gate_code, gate_up, preferred_element_type=jnp.float32) + gate_bias
    decay_logarithm = (jax.nn.log_sigmoid(gate_score) / softness_divisor).reshape(
        segment_count, SEGMENT_LENGTH, head_count, KEY_WIDTH
    )
    inside = jnp.cumsum(decay_logarithm, axis=1)
    seg_total = inside[:, -1]
    key_blocks = keys.reshape(segment_count, SEGMENT_LENGTH, head_count, KEY_WIDTH)
    scaled_keys = (key_blocks * jnp.exp(seg_total[:, None] - inside)).astype(jnp.bfloat16)
    value_blocks = values.reshape(segment_count, SEGMENT_LENGTH, head_count, HEAD_V)
    update = jnp.einsum(
        "nshk,nshv->nhkv", scaled_keys, value_blocks, preferred_element_type=jnp.float32
    )
    through, local_state = lax.associative_scan(chain, (jnp.exp(seg_total), update), axis=0)
    device_decay = through[-1]
    device_state = local_state[-1]
    columns = lax.all_to_all(
        device_state[None].astype(jnp.bfloat16), "sp", split_axis=3, concat_axis=0, tiled=True
    ).astype(jnp.float32)
    decays = lax.all_gather(device_decay[None], "sp", axis=0, tiled=True)
    running = lax.associative_scan(chain, (decays, columns), axis=0)[1]
    before = jnp.concatenate([jnp.zeros_like(running[:1]), running[:-1]], axis=0)
    incoming = lax.all_to_all(
        for_sending(before), "sp", split_axis=0, concat_axis=3, tiled=True
    ).astype(before.dtype)[0]
    states = local_state + through[..., None] * incoming[None]
    query_blocks = queries.reshape(segment_count, SEGMENT_LENGTH, head_count, KEY_WIDTH)
    readout = jnp.einsum(
        "nshk,nhkv->nshv",
        query_blocks,
        states.astype(jnp.bfloat16),
        preferred_element_type=jnp.float32,
    )
    norm_scale = lax.rsqrt(jnp.mean(readout * readout, axis=-1, keepdims=True) + epsilon)
    gla_mix = (
        (readout * norm_scale * gla_gain)
        .astype(jnp.bfloat16)
        .reshape(row_count, head_count * HEAD_V)
    )
    reach_rows = conv_taps.shape[0] - 1
    earlier_rows = from_behind(conv_input[row_count - reach_rows :], "sp", 1)
    extended = jnp.concatenate([earlier_rows, conv_input], axis=0)
    convolved = jnp.zeros(conv_input.shape, jnp.float32)
    for offset in range(reach_rows + 1):
        convolved = convolved + conv_taps[offset] * extended[offset : offset + row_count]
    conv_mix = (conv_gate * convolved).astype(jnp.bfloat16)
    wide_gla, wide_conv = (
        lax.all_gather(out_gla, "sp", axis=1, tiled=True),
        lax.all_gather(out_conv, "sp", axis=1, tiled=True),
    )
    summed = jnp.dot(gla_mix, wide_gla, preferred_element_type=jnp.float32)
    return lax.psum_scatter(
        (summed + jnp.dot(conv_mix, wide_conv, preferred_element_type=jnp.float32)).astype(
            jnp.bfloat16
        ),
        "tp",
        scatter_dimension=0,
        tiled=True,
    )


MESH = pl.DeviceIdType.MESH
ARGS = 12
LANES = 128
HALO = 16
CHUNKS = 2
SPLIT = 2
BITS = 3


def flipped(index, bit):
    return index + bit - 2 * bit * ((index // bit) % 2)


def fits(mesh):
    return mesh.shape["sp"] == SPLIT**BITS and mesh.shape["tp"] == SPLIT**2


def kernel(
    n_sp,
    n_tp,
    *refs,
):
    sources, out_ref, scratch = refs[:ARGS], refs[ARGS], refs[ARGS + 1 :]
    held, scratch = scratch[:ARGS], scratch[ARGS:]
    body(n_sp, n_tp, sources, held, out_ref, *scratch)


def body(
    n_sp,
    n_tp,
    sources,
    held,
    out_ref,
    in_sem,
    halo,
    ext,
    st,
    dec,
    cols,
    bef,
    inc,
    sloc,
    thr,
    mix,
    wbuf,
    cbuf,
    mrecv,
    csum,
    crecv,
    halo_sem,
    a_sem,
    d_sem,
    b_sem,
    w_sem,
    mix_sem,
    m_sem,
    c_sem,
):
    (
        q_ref,
        k_ref,
        v_ref,
        code_ref,
        up_ref,
        bias_ref,
        gain_ref,
        x_ref,
        cg_ref,
        taps_ref,
        wg_ref,
        wc_ref,
    ) = held
    loads = [pltpu.make_async_copy(a, b, in_sem.at[i]) for i, (a, b) in enumerate(zip(sources, held))]
    loading = list(range(ARGS))

    def need(*which):
        for i in which:
            loads[i].wait()
            loading.remove(i)

    for i in (7, 11, 3, 4, 5, 1, 2, 10, 8, 9, 0, 6):
        loads[i].start()
    s, t = lax.axis_index("sp"), lax.axis_index("tp")
    f32, bf16 = jnp.float32, jnp.bfloat16
    rows, key_cols = q_ref.shape
    seg = SEGMENT_LENGTH
    segs = rows // seg
    heads = key_cols // KEY_WIDTH
    val_rows = HEAD_V // n_sp
    chan, width = wg_ref.shape
    piece = rows // n_tp
    started = []

    def send(src, dst, sems, where):
        copy = pltpu.make_async_remote_copy(
            src_ref=src,
            dst_ref=dst,
            send_sem=sems[0],
            recv_sem=sems[1],
            device_id=where,
            device_id_type=MESH,
        )
        copy.start()
        started.append(copy)
        return copy

    def pair(sem, *index):
        return sem.at[(0, *index)], sem.at[(1, *index)]

    side, low, far = flipped(s, 1), flipped(s, 2), flipped(s, 4)

    barrier = pltpu.get_barrier_semaphore()
    greet = [(lax.rem(s + d, n_sp), t) for d in range(1, n_sp)]
    mate, across = flipped(t, 1), flipped(t, 2)
    greet += [(s, mate), (s, across), (low, across)]
    for where in greet:
        pl.semaphore_signal(barrier, inc=1, device_id=where, device_id_type=MESH)

    weight = (wc_ref, wg_ref)
    step = chan // CHUNKS
    to_side, to_far, onward = {}, {}, {}

    def over_side(half, c):
        part = pl.ds(c * step, step)
        to_side[half, c] = send(
            weight[half].at[part], wbuf.at[half, 0, part], pair(w_sem, 0, half, c), (side, t)
        )

    for half in range(2):
        for c in range(CHUNKS):
            part = pl.ds(c * step, step)
            send_sem, recv_sem = pair(w_sem, 1, half, c)
            to_far[half, c] = pltpu.make_async_remote_copy(
                src_ref=weight[half].at[part],
                dst_ref=wbuf.at[half, 1, part],
                send_sem=send_sem,
                recv_sem=recv_sem,
                device_id=(far, t),
                device_id_type=MESH,
            )
            started.append(to_far[half, c])

    inner = (s // 2) % 2 != s // 4

    def inner_far(*chunks):
        @pl.when(inner)
        def _():
            for chunk in chunks:
                to_far[chunk].start()

    def outer_far(*chunks):
        @pl.when(jnp.logical_not(inner))
        def _():
            for chunk in chunks:
                to_far[chunk].start()

    def pass_on(half, c):
        part = pl.ds(c * step, step)
        to_far[half, c].wait_recv()
        onward[half, c] = send(
            wbuf.at[half, 1, part], wbuf.at[half, 2, part], pair(w_sem, 2, half, c), (side, t)
        )

    need(3, 4, 5, 1, 2)
    g = (
        lax.dot_general(
            code_ref[...],
            up_ref[...],
            (((0,), (0,)), ((), ())),
            preferred_element_type=f32,
        )
        + bias_ref[...]
    )
    log_decay = (jnp.minimum(g, 0.0) - jnp.log1p(jnp.exp(-jnp.abs(g)))) / softness_divisor
    row_i = lax.broadcasted_iota(jnp.int32, (seg, seg), 0)
    col_i = lax.broadcasted_iota(jnp.int32, (seg, seg), 1)
    later = (col_i > row_i).astype(f32)
    state = None
    passed = None
    for n in range(segs):
        here = pl.ds(n * seg, seg)
        block = log_decay[n * seg : (n + 1) * seg]
        rest = jnp.dot(
            later, block, preferred_element_type=f32, precision=lax.Precision.HIGHEST
        )
        total = jnp.sum(block, axis=0, keepdims=True)
        scaled = (k_ref[here, :].astype(f32) * jnp.exp(rest)).astype(bf16)
        update = jnp.concatenate(
            [
                lax.dot_general(
                    v_ref[here, pl.ds(h * HEAD_V, HEAD_V)],
                    scaled[:, h * KEY_WIDTH : (h + 1) * KEY_WIDTH],
                    (((0,), (0,)), ((), ())),
                    preferred_element_type=f32,
                )
                for h in range(heads)
            ],
            axis=1,
        )
        if n == 0:
            state, passed = update, total
        else:
            state, passed = jnp.exp(total) * state + update, passed + total
        sloc[n] = state
        thr[n] = jnp.exp(passed)
    st[...] = state.astype(bf16).reshape(st.shape)
    dec[s] = jnp.exp(passed)
    cols[s] = st[s]

    pl.semaphore_wait(barrier, len(greet))
    need(7, 11)
    halo_copy = send(
        x_ref.at[pl.ds(rows - HALO, HALO)], halo, pair(halo_sem), (lax.rem(s + 1, n_sp), t)
    )
    first = []
    for d in range(1, n_sp):
        dst = lax.rem(s + d, n_sp)
        first.append(send(st.at[dst], cols.at[s], pair(a_sem, d - 1), (dst, t)))
        first.append(send(dec.at[s], dec.at[s], pair(d_sem, d - 1), (dst, t)))

    to_far[0, 0].start()
    over_side(0, 0)
    over_side(0, 1)
    inner_far((0, 1))

    halo_copy.wait_recv()
    need(8, 9)
    ext[pl.ds(0, HALO), :] = jnp.where(s > 0, halo[...].astype(f32), 0.0)
    ext[pl.ds(HALO, rows), :] = x_ref[...].astype(f32)
    taps = taps_ref.shape[0]
    total = None
    for o in range(taps):
        term = taps_ref[pl.ds(o, 1), :] * ext[pl.ds(HALO - taps + 1 + o, rows), :]
        total = term if total is None else total + term
    mix[0, 0] = (cg_ref[...].astype(f32) * total).astype(bf16)

    for copy in first:
        copy.wait_recv()
    running = jnp.zeros(cols.shape[1:], f32)
    for j in range(n_sp):
        bef[j] = running.astype(bf16)
        if j < n_sp - 1:
            running = dec[j] * running + cols[j].astype(f32)
    inc[s] = bef[s]
    second = []
    for d in range(1, n_sp):
        dst = lax.rem(s + d, n_sp)
        second.append(send(bef.at[dst], inc.at[s], pair(b_sem, d - 1), (dst, t)))

    need(10, 0, 6)
    for c in range(CHUNKS):
        over_side(1, c)
    inner_far(*((1, c) for c in range(CHUNKS)))
    mix_copies = {0: send(mix.at[0, 0], mix.at[1, 0], pair(mix_sem, 0), (low, t))}
    pass_on(0, 0)

    for copy in second:
        copy.wait_recv()
    incoming = inc[...].astype(f32).reshape(HEAD_V, key_cols)
    for n in range(segs):
        here = pl.ds(n * seg, seg)
        full = (sloc[n] + thr[n] * incoming).astype(bf16)
        for h in range(heads):
            lanes = slice(h * KEY_WIDTH, (h + 1) * KEY_WIDTH)
            read = lax.dot_general(
                q_ref[here, lanes],
                full[:, lanes],
                (((1,), (1,)), ((), ())),
                preferred_element_type=f32,
            )
            scale = lax.rsqrt(jnp.mean(read * read, axis=-1, keepdims=True) + epsilon)
            mix[0, 1, here, pl.ds(h * HEAD_V, HEAD_V)] = (
                read * scale * gain_ref[...]
            ).astype(bf16)
    mix_copies[1] = send(mix.at[0, 1], mix.at[1, 1], pair(mix_sem, 1), (low, t))
    outer_far((0, 1), *((1, c) for c in range(CHUNKS)))

    halves, results = {}, {}

    def rows_of(owner):
        return pl.ds(pl.multiple_of(owner * piece, piece), piece)

    def product(whose, slot):
        acc = None
        for half in range(2):
            w = weight[half][...] if slot == 0 else wbuf[half, slot - 1]
            term = jnp.dot(mix[whose, half], w, preferred_element_type=f32)
            acc = term if acc is None else acc + term
        cbuf[whose, slot] = acc.astype(bf16)
        for dy in (1, 0):
            owner = flipped(across, 1) if dy else mate
            halves[whose, slot, dy] = send(
                cbuf.at[whose, slot, rows_of(owner)],
                mrecv.at[whose, slot, dy],
                pair(m_sem, whose, slot, dy),
                (s, mate),
            )

    def finish(whose, slot):
        for dy in (1, 0):
            owner = across if dy else t
            halves[whose, slot, dy].wait_recv()
            both = cbuf[whose, slot, rows_of(owner), :].astype(f32) + mrecv[
                whose, slot, dy
            ].astype(f32)
            csum[whose, slot, dy] = both.astype(bf16)
            if whose or dy:
                results[whose, slot, dy] = send(
                    csum.at[whose, slot, dy],
                    crecv.at[whose, slot, dy],
                    pair(c_sem, whose, slot, dy),
                    (low if whose else s, owner),
                )

    product(0, 0)
    for half in range(2):
        for c in range(CHUNKS):
            to_side[half, c].wait_recv()
    product(0, 1)
    finish(0, 0)
    finish(0, 1)
    for c in range(1, CHUNKS):
        pass_on(0, c)
    for half in range(2):
        mix_copies[half].wait_recv()
    product(1, 0)
    product(1, 1)
    finish(1, 0)
    finish(1, 1)
    for c in range(CHUNKS):
        pass_on(1, c)
    product(1, 2)
    product(0, 2)
    finish(1, 2)
    finish(0, 2)
    for half in range(2):
        for c in range(CHUNKS):
            onward[half, c].wait_recv()
    product(1, 3)
    product(0, 3)
    finish(1, 3)
    finish(0, 3)

    for slot in range(4):
        for whose in range(2):
            results[whose, slot, 1].wait_recv()
            if whose:
                results[1, slot, 0].wait_recv()
                total = crecv[1, slot, 0].astype(f32)
            else:
                total = csum[0, slot, 0].astype(f32)
            total = total + crecv[whose, slot, 1].astype(f32)
            block = low if whose else s
            if slot % 2:
                block = flipped(block, 1)
            if slot // 2:
                block = flipped(block, 4)
            place = pl.ds(pl.multiple_of(block * width, width), width)
            out_ref[:, place] = total.astype(bf16)
    for copy in started:
        copy.wait_send()


def fused(
    queries,
    keys,
    values,
    gate_code,
    gate_up,
    gate_bias,
    gla_gain,
    conv_input,
    conv_gate,
    conv_taps,
    out_gla,
    out_conv,
):
    n_sp, n_tp = lax.axis_size("sp"), lax.axis_size("tp")
    rows, key_cols = queries.shape
    segs = rows // SEGMENT_LENGTH
    chan, width = out_gla.shape
    bf16, f32 = jnp.bfloat16, jnp.float32
    val_rows = HEAD_V // n_sp
    dma = pltpu.SemaphoreType.DMA
    operands = (
        queries,
        keys,
        values,
        gate_code.T,
        gate_up,
        gate_bias[None],
        gla_gain[None],
        conv_input,
        conv_gate,
        conv_taps,
        out_gla,
        out_conv,
    )
    return pl.pallas_call(
        functools.partial(kernel, n_sp, n_tp),
        out_shape=jax.ShapeDtypeStruct((rows // n_tp, n_sp * width), bf16),
        in_specs=[pl.BlockSpec(memory_space=pltpu.HBM)] * ARGS,
        out_specs=pl.BlockSpec(memory_space=pltpu.VMEM),
        scratch_shapes=[
            *(pltpu.VMEM(a.shape, a.dtype) for a in operands),
            dma((ARGS,)),
            pltpu.VMEM((HALO, conv_input.shape[1]), bf16),
            pltpu.VMEM((HALO + rows, conv_input.shape[1]), f32),
            pltpu.VMEM((n_sp, val_rows, key_cols), bf16),
            pltpu.VMEM((n_sp, 1, key_cols), f32),
            pltpu.VMEM((n_sp, val_rows, key_cols), bf16),
            pltpu.VMEM((n_sp, val_rows, key_cols), bf16),
            pltpu.VMEM((n_sp, val_rows, key_cols), bf16),
            pltpu.VMEM((segs, HEAD_V, key_cols), f32),
            pltpu.VMEM((segs, 1, key_cols), f32),
            pltpu.VMEM((2, 2, rows, chan), bf16),
            pltpu.VMEM((2, 3, chan, width), bf16),
            pltpu.VMEM((2, 4, rows, width), bf16),
            pltpu.VMEM((2, 4, 2, rows // n_tp, width), bf16),
            pltpu.VMEM((2, 4, 2, rows // n_tp, width), bf16),
            pltpu.VMEM((2, 4, 2, rows // n_tp, width), bf16),
            dma((2,)),
            dma((2, n_sp - 1)),
            dma((2, n_sp - 1)),
            dma((2, n_sp - 1)),
            dma((2, 3, 2, CHUNKS)),
            dma((2, 2)),
            dma((2, 2, 4, 2)),
            dma((2, 2, 4, 2)),
        ],
        compiler_params=pltpu.CompilerParams(
            collective_id=0, has_side_effects=True, vmem_limit_bytes=67043328
        ),
    )(*operands)


def solution(mesh):
    in_specs = (
        P("sp", "tp"),
        P("sp", "tp"),
        P("sp", "tp"),
        P("sp", None),
        P(None, "tp"),
        P("tp"),
        P(),
        P("sp", "tp"),
        P("sp", "tp"),
        P(None, "tp"),
        P("tp", "sp"),
        P("tp", "sp"),
    )
    out_specs = P(("sp", "tp"), None)
    return jax.shard_map(
        fused if fits(mesh) else per_device, mesh=mesh, in_specs=in_specs, out_specs=out_specs, check_vma=False
    )
```

```python
import functools

import jax
import jax.numpy as jnp
from jax import lax
from jax.experimental import pallas as pl
from jax.experimental.pallas import tpu as pltpu
from jax.sharding import PartitionSpec as P

KEY_WIDTH = 128
HEAD_V = 256
SEGMENT_LENGTH = 64


softness_divisor = 16.0
epsilon = 1.0


def for_sending(x):
    return jax.tree.map(lambda a: a.astype(jnp.bfloat16) if a.dtype == jnp.float32 else a, x)


def from_behind(x, axis, by):
    count = lax.axis_size(axis)
    pairs = [(i, i + by) for i in range(count) if 0 <= i + by < count]
    return lax.ppermute(x, axis, pairs)


def chain(earlier, latter):
    return (earlier[0] * latter[0], latter[0][..., None] * earlier[1] + latter[1])


def per_device(
    queries,
    keys,
    values,
    gate_code,
    gate_up,
    gate_bias,
    gla_gain,
    conv_input,
    conv_gate,
    conv_taps,
    out_gla,
    out_conv,
):
    row_count = queries.shape[0]
    segment_count = row_count // SEGMENT_LENGTH
    head_count = queries.shape[1] // KEY_WIDTH
    gate_score = jnp.dot(gate_code, gate_up, preferred_element_type=jnp.float32) + gate_bias
    decay_logarithm = (jax.nn.log_sigmoid(gate_score) / softness_divisor).reshape(
        segment_count, SEGMENT_LENGTH, head_count, KEY_WIDTH
    )
    inside = jnp.cumsum(decay_logarithm, axis=1)
    seg_total = inside[:, -1]
    key_blocks = keys.reshape(segment_count, SEGMENT_LENGTH, head_count, KEY_WIDTH)
    scaled_keys = (key_blocks * jnp.exp(seg_total[:, None] - inside)).astype(jnp.bfloat16)
    value_blocks = values.reshape(segment_count, SEGMENT_LENGTH, head_count, HEAD_V)
    update = jnp.einsum(
        "nshk,nshv->nhkv", scaled_keys, value_blocks, preferred_element_type=jnp.float32
    )
    through, local_state = lax.associative_scan(chain, (jnp.exp(seg_total), update), axis=0)
    device_decay = through[-1]
    device_state = local_state[-1]
    columns = lax.all_to_all(
        device_state[None].astype(jnp.bfloat16), "sp", split_axis=3, concat_axis=0, tiled=True
    ).astype(jnp.float32)
    decays = lax.all_gather(device_decay[None], "sp", axis=0, tiled=True)
    running = lax.associative_scan(chain, (decays, columns), axis=0)[1]
    before = jnp.concatenate([jnp.zeros_like(running[:1]), running[:-1]], axis=0)
    incoming = lax.all_to_all(
        for_sending(before), "sp", split_axis=0, concat_axis=3, tiled=True
    ).astype(before.dtype)[0]
    states = local_state + through[..., None] * incoming[None]
    query_blocks = queries.reshape(segment_count, SEGMENT_LENGTH, head_count, KEY_WIDTH)
    readout = jnp.einsum(
        "nshk,nhkv->nshv",
        query_blocks,
        states.astype(jnp.bfloat16),
        preferred_element_type=jnp.float32,
    )
    norm_scale = lax.rsqrt(jnp.mean(readout * readout, axis=-1, keepdims=True) + epsilon)
    gla_mix = (
        (readout * norm_scale * gla_gain)
        .astype(jnp.bfloat16)
        .reshape(row_count, head_count * HEAD_V)
    )
    reach_rows = conv_taps.shape[0] - 1
    earlier_rows = from_behind(conv_input[row_count - reach_rows :], "sp", 1)
    extended = jnp.concatenate([earlier_rows, conv_input], axis=0)
    convolved = jnp.zeros(conv_input.shape, jnp.float32)
    for offset in range(reach_rows + 1):
        convolved = convolved + conv_taps[offset] * extended[offset : offset + row_count]
    conv_mix = (conv_gate * convolved).astype(jnp.bfloat16)
    wide_gla, wide_conv = (
        lax.all_gather(out_gla, "sp", axis=1, tiled=True),
        lax.all_gather(out_conv, "sp", axis=1, tiled=True),
    )
    summed = jnp.dot(gla_mix, wide_gla, preferred_element_type=jnp.float32)
    return lax.psum_scatter(
        (summed + jnp.dot(conv_mix, wide_conv, preferred_element_type=jnp.float32)).astype(
            jnp.bfloat16
        ),
        "tp",
        scatter_dimension=0,
        tiled=True,
    )


MESH = pl.DeviceIdType.MESH
ARGS = 12
LANES = 128
HALO = 16
CHUNKS = 2
SPLIT = 2
BITS = 3


def flipped(index, bit):
    return index + bit - 2 * bit * ((index // bit) % 2)


def fits(mesh):
    return mesh.shape["sp"] == SPLIT**BITS and mesh.shape["tp"] == SPLIT**2


def kernel(
    n_sp,
    n_tp,
    *refs,
):
    sources, out_ref, scratch = refs[:ARGS], refs[ARGS], refs[ARGS + 1 :]
    held, scratch = scratch[:ARGS], scratch[ARGS:]
    body(n_sp, n_tp, sources, held, out_ref, *scratch)


def body(
    n_sp,
    n_tp,
    sources,
    held,
    out_ref,
    in_sem,
    halo,
    ext,
    st,
    dec,
    cols,
    bef,
    inc,
    sloc,
    thr,
    mix,
    wbuf,
    cbuf,
    mrecv,
    csum,
    crecv,
    halo_sem,
    a_sem,
    d_sem,
    b_sem,
    w_sem,
    mix_sem,
    m_sem,
    c_sem,
):
    (
        q_ref,
        k_ref,
        v_ref,
        code_ref,
        up_ref,
        bias_ref,
        gain_ref,
        x_ref,
        cg_ref,
        taps_ref,
        wg_ref,
        wc_ref,
    ) = held
    loads = [pltpu.make_async_copy(a, b, in_sem.at[i]) for i, (a, b) in enumerate(zip(sources, held))]
    loading = list(range(ARGS))

    def need(*which):
        for i in which:
            loads[i].wait()
            loading.remove(i)

    for i in (7, 11, 3, 4, 5, 1, 2, 10, 8, 9, 0, 6):
        loads[i].start()
    s, t = lax.axis_index("sp"), lax.axis_index("tp")
    f32, bf16 = jnp.float32, jnp.bfloat16
    rows, key_cols = q_ref.shape
    seg = SEGMENT_LENGTH
    segs = rows // seg
    heads = key_cols // KEY_WIDTH
    val_rows = HEAD_V // n_sp
    chan, width = wg_ref.shape
    piece = rows // n_tp
    started = []

    def send(src, dst, sems, where):
        copy = pltpu.make_async_remote_copy(
            src_ref=src,
            dst_ref=dst,
            send_sem=sems[0],
            recv_sem=sems[1],
            device_id=where,
            device_id_type=MESH,
        )
        copy.start()
        started.append(copy)
        return copy

    def pair(sem, *index):
        return sem.at[(0, *index)], sem.at[(1, *index)]

    side, low, far = flipped(s, 1), flipped(s, 2), flipped(s, 4)

    barrier = pltpu.get_barrier_semaphore()
    greet = [(lax.rem(s + d, n_sp), t) for d in range(1, n_sp)]
    mate, across = flipped(t, 1), flipped(t, 2)
    greet += [(s, mate), (s, across), (low, across)]
    for where in greet:
        pl.semaphore_signal(barrier, inc=1, device_id=where, device_id_type=MESH)

    weight = (wc_ref, wg_ref)
    step = chan // CHUNKS
    to_side, to_far, onward = {}, {}, {}

    def over_side(half, c):
        part = pl.ds(c * step, step)
        to_side[half, c] = send(
            weight[half].at[part], wbuf.at[half, 0, part], pair(w_sem, 0, half, c), (side, t)
        )

    for half in range(2):
        for c in range(CHUNKS):
            part = pl.ds(c * step, step)
            send_sem, recv_sem = pair(w_sem, 1, half, c)
            to_far[half, c] = pltpu.make_async_remote_copy(
                src_ref=weight[half].at[part],
                dst_ref=wbuf.at[half, 1, part],
                send_sem=send_sem,
                recv_sem=recv_sem,
                device_id=(far, t),
                device_id_type=MESH,
            )
            started.append(to_far[half, c])

    inner = (s // 2) % 2 != s // 4

    def inner_far(*chunks):
        @pl.when(inner)
        def _():
            for chunk in chunks:
                to_far[chunk].start()

    def outer_far(*chunks):
        @pl.when(jnp.logical_not(inner))
        def _():
            for chunk in chunks:
                to_far[chunk].start()

    def pass_on(half, c):
        part = pl.ds(c * step, step)
        to_far[half, c].wait_recv()
        onward[half, c] = send(
            wbuf.at[half, 1, part], wbuf.at[half, 2, part], pair(w_sem, 2, half, c), (side, t)
        )

    need(3, 4, 5, 1, 2)
    g = (
        lax.dot_general(
            code_ref[...],
            up_ref[...],
            (((0,), (0,)), ((), ())),
            preferred_element_type=f32,
        )
        + bias_ref[...]
    )
    log_decay = (jnp.minimum(g, 0.0) - jnp.log1p(jnp.exp(-jnp.abs(g)))) / softness_divisor
    row_i = lax.broadcasted_iota(jnp.int32, (seg, seg), 0)
    col_i = lax.broadcasted_iota(jnp.int32, (seg, seg), 1)
    later = (col_i > row_i).astype(f32)
    state = None
    passed = None
    for n in range(segs):
        here = pl.ds(n * seg, seg)
        block = log_decay[n * seg : (n + 1) * seg]
        rest = jnp.dot(
            later, block, preferred_element_type=f32, precision=lax.Precision.HIGHEST
        )
        total = jnp.sum(block, axis=0, keepdims=True)
        scaled = (k_ref[here, :].astype(f32) * jnp.exp(rest)).astype(bf16)
        update = jnp.concatenate(
            [
                lax.dot_general(
                    v_ref[here, pl.ds(h * HEAD_V, HEAD_V)],
                    scaled[:, h * KEY_WIDTH : (h + 1) * KEY_WIDTH],
                    (((0,), (0,)), ((), ())),
                    preferred_element_type=f32,
                )
                for h in range(heads)
            ],
            axis=1,
        )
        if n == 0:
            state, passed = update, total
        else:
            state, passed = jnp.exp(total) * state + update, passed + total
        sloc[n] = state
        thr[n] = jnp.exp(passed)
    st[...] = state.astype(bf16).reshape(st.shape)
    dec[s] = jnp.exp(passed)
    cols[s] = st[s]

    pl.semaphore_wait(barrier, len(greet))
    need(7, 11)
    halo_copy = send(
        x_ref.at[pl.ds(rows - HALO, HALO)], halo, pair(halo_sem), (lax.rem(s + 1, n_sp), t)
    )
    first = []
    for d in range(1, n_sp):
        dst = lax.rem(s + d, n_sp)
        first.append(send(st.at[dst], cols.at[s], pair(a_sem, d - 1), (dst, t)))
        first.append(send(dec.at[s], dec.at[s], pair(d_sem, d - 1), (dst, t)))

    inner_far((0, 0))
    over_side(0, 0)

    halo_copy.wait_recv()
    need(8, 9)
    ext[pl.ds(0, HALO), :] = jnp.where(s > 0, halo[...].astype(f32), 0.0)
    ext[pl.ds(HALO, rows), :] = x_ref[...].astype(f32)
    taps = taps_ref.shape[0]
    total = None
    for o in range(taps):
        term = taps_ref[pl.ds(o, 1), :] * ext[pl.ds(HALO - taps + 1 + o, rows), :]
        total = term if total is None else total + term
    mix[0, 0] = (cg_ref[...].astype(f32) * total).astype(bf16)

    for copy in first:
        copy.wait_recv()
    running = jnp.zeros(cols.shape[1:], f32)
    for j in range(n_sp):
        bef[j] = running.astype(bf16)
        if j < n_sp - 1:
            running = dec[j] * running + cols[j].astype(f32)
    inc[s] = bef[s]
    second = []
    for d in range(1, n_sp):
        dst = lax.rem(s + d, n_sp)
        second.append(send(bef.at[dst], inc.at[s], pair(b_sem, d - 1), (dst, t)))

    need(10, 0, 6)
    over_side(0, 1)
    inner_far((0, 1))
    for c in range(CHUNKS):
        over_side(1, c)
    inner_far(*((1, c) for c in range(CHUNKS)))
    mix_copies = {0: send(mix.at[0, 0], mix.at[1, 0], pair(mix_sem, 0), (low, t))}

    for copy in second:
        copy.wait_recv()
    incoming = inc[...].astype(f32).reshape(HEAD_V, key_cols)
    for n in range(segs):
        here = pl.ds(n * seg, seg)
        full = (sloc[n] + thr[n] * incoming).astype(bf16)
        for h in range(heads):
            lanes = slice(h * KEY_WIDTH, (h + 1) * KEY_WIDTH)
            read = lax.dot_general(
                q_ref[here, lanes],
                full[:, lanes],
                (((1,), (1,)), ((), ())),
                preferred_element_type=f32,
            )
            scale = lax.rsqrt(jnp.mean(read * read, axis=-1, keepdims=True) + epsilon)
            mix[0, 1, here, pl.ds(h * HEAD_V, HEAD_V)] = (
                read * scale * gain_ref[...]
            ).astype(bf16)
    mix_copies[1] = send(mix.at[0, 1], mix.at[1, 1], pair(mix_sem, 1), (low, t))
    outer_far(*((h, c) for h in range(2) for c in range(CHUNKS)))

    halves, results = {}, {}

    def rows_of(owner):
        return pl.ds(pl.multiple_of(owner * piece, piece), piece)

    def product(whose, slot):
        acc = None
        for half in range(2):
            w = weight[half][...] if slot == 0 else wbuf[half, slot - 1]
            term = jnp.dot(mix[whose, half], w, preferred_element_type=f32)
            acc = term if acc is None else acc + term
        cbuf[whose, slot] = acc.astype(bf16)
        for dy in (1, 0):
            owner = flipped(across, 1) if dy else mate
            halves[whose, slot, dy] = send(
                cbuf.at[whose, slot, rows_of(owner)],
                mrecv.at[whose, slot, dy],
                pair(m_sem, whose, slot, dy),
                (s, mate),
            )

    def finish(whose, slot):
        for dy in (1, 0):
            owner = across if dy else t
            halves[whose, slot, dy].wait_recv()
            both = cbuf[whose, slot, rows_of(owner), :].astype(f32) + mrecv[
                whose, slot, dy
            ].astype(f32)
            csum[whose, slot, dy] = both.astype(bf16)
            if whose or dy:
                results[whose, slot, dy] = send(
                    csum.at[whose, slot, dy],
                    crecv.at[whose, slot, dy],
                    pair(c_sem, whose, slot, dy),
                    (low if whose else s, owner),
                )

    product(0, 0)
    for half in range(2):
        for c in range(CHUNKS):
            to_side[half, c].wait_recv()
    product(0, 1)
    finish(0, 0)
    finish(0, 1)
    for c in range(CHUNKS):
        pass_on(0, c)
    for half in range(2):
        mix_copies[half].wait_recv()
    product(1, 0)
    product(1, 1)
    finish(1, 0)
    finish(1, 1)
    for c in range(CHUNKS):
        pass_on(1, c)
    product(1, 2)
    product(0, 2)
    finish(1, 2)
    finish(0, 2)
    for half in range(2):
        for c in range(CHUNKS):
            onward[half, c].wait_recv()
    product(1, 3)
    product(0, 3)
    finish(1, 3)
    finish(0, 3)

    for slot in range(4):
        for whose in range(2):
            results[whose, slot, 1].wait_recv()
            if whose:
                results[1, slot, 0].wait_recv()
                total = crecv[1, slot, 0].astype(f32)
            else:
                total = csum[0, slot, 0].astype(f32)
            total = total + crecv[whose, slot, 1].astype(f32)
            block = low if whose else s
            if slot % 2:
                block = flipped(block, 1)
            if slot // 2:
                block = flipped(block, 4)
            place = pl.ds(pl.multiple_of(block * width, width), width)
            out_ref[:, place] = total.astype(bf16)
    for copy in started:
        copy.wait_send()


def fused(
    queries,
    keys,
    values,
    gate_code,
    gate_up,
    gate_bias,
    gla_gain,
    conv_input,
    conv_gate,
    conv_taps,
    out_gla,
    out_conv,
):
    n_sp, n_tp = lax.axis_size("sp"), lax.axis_size("tp")
    rows, key_cols = queries.shape
    segs = rows // SEGMENT_LENGTH
    chan, width = out_gla.shape
    bf16, f32 = jnp.bfloat16, jnp.float32
    val_rows = HEAD_V // n_sp
    dma = pltpu.SemaphoreType.DMA
    operands = (
        queries,
        keys,
        values,
        gate_code.T,
        gate_up,
        gate_bias[None],
        gla_gain[None],
        conv_input,
        conv_gate,
        conv_taps,
        out_gla,
        out_conv,
    )
    return pl.pallas_call(
        functools.partial(kernel, n_sp, n_tp),
        out_shape=jax.ShapeDtypeStruct((rows // n_tp, n_sp * width), bf16),
        in_specs=[pl.BlockSpec(memory_space=pltpu.HBM)] * ARGS,
        out_specs=pl.BlockSpec(memory_space=pltpu.VMEM),
        scratch_shapes=[
            *(pltpu.VMEM(a.shape, a.dtype) for a in operands),
            dma((ARGS,)),
            pltpu.VMEM((HALO, conv_input.shape[1]), bf16),
            pltpu.VMEM((HALO + rows, conv_input.shape[1]), f32),
            pltpu.VMEM((n_sp, val_rows, key_cols), bf16),
            pltpu.VMEM((n_sp, 1, key_cols), f32),
            pltpu.VMEM((n_sp, val_rows, key_cols), bf16),
            pltpu.VMEM((n_sp, val_rows, key_cols), bf16),
            pltpu.VMEM((n_sp, val_rows, key_cols), bf16),
            pltpu.VMEM((segs, HEAD_V, key_cols), f32),
            pltpu.VMEM((segs, 1, key_cols), f32),
            pltpu.VMEM((2, 2, rows, chan), bf16),
            pltpu.VMEM((2, 3, chan, width), bf16),
            pltpu.VMEM((2, 4, rows, width), bf16),
            pltpu.VMEM((2, 4, 2, rows // n_tp, width), bf16),
            pltpu.VMEM((2, 4, 2, rows // n_tp, width), bf16),
            pltpu.VMEM((2, 4, 2, rows // n_tp, width), bf16),
            dma((2,)),
            dma((2, n_sp - 1)),
            dma((2, n_sp - 1)),
            dma((2, n_sp - 1)),
            dma((2, 3, 2, CHUNKS)),
            dma((2, 2)),
            dma((2, 2, 4, 2)),
            dma((2, 2, 4, 2)),
        ],
        compiler_params=pltpu.CompilerParams(
            collective_id=0, has_side_effects=True, vmem_limit_bytes=67043328
        ),
    )(*operands)


def solution(mesh):
    in_specs = (
        P("sp", "tp"),
        P("sp", "tp"),
        P("sp", "tp"),
        P("sp", None),
        P(None, "tp"),
        P("tp"),
        P(),
        P("sp", "tp"),
        P("sp", "tp"),
        P(None, "tp"),
        P("tp", "sp"),
        P("tp", "sp"),
    )
    out_specs = P(("sp", "tp"), None)
    return jax.shard_map(
        fused if fits(mesh) else per_device, mesh=mesh, in_specs=in_specs, out_specs=out_specs, check_vma=False
    )
```
